32 devices in a mesh: grp: 2 (over y), ep: 4 (over z), tp: 4 (over x, core).
Axes of the slice: x: 2, y: 2, z: 4, core: 2. Of those that a mesh axis runs over, the one named last changes fastest.
Arguments:
- hidden_in: bfloat16 [4096, 2048], P(('grp', 'ep', 'tp')), parts along dimension 0, may hold values from -6 to 6
- expert_ids: int32 [4096, 2], P(('grp', 'ep', 'tp')), parts along dimension 0, may hold values from 0 to 15, all different within a row; in each aligned block of 128 rows (0 to 127, 128 to 255, ...) at most 32 rows name the same one
- route_weights: float32 [4096, 2], P(('grp', 'ep', 'tp')), parts along dimension 0, may hold values from 0.1 to 1
- norm_gain: float32 [2048], replicated, may hold values from 0.1 to 1.9
- gate_proj: bfloat16 [16, 2048, 512], P(('ep', 'tp')), may hold values from -0.125 to 0.125
- up_proj: bfloat16 [16, 2048, 512], P(('ep', 'tp')), may hold values from -0.125 to 0.125
- down_proj: bfloat16 [16, 512, 2048], P(('ep', 'tp')), may hold values from -0.25 to 0.25
Outputs:
- mixed_out: bfloat16 [4096, 2048], P(('grp', 'ep', 'tp')), parts along dimension 0
The draws below stay inside these ranges and needn't reach their ends.
There are 2 independent parts, one for each index of `grp`. The reference program is written for one: setup_inputs(seed, part) draws one part's arguments, and reference() takes and returns one part's arrays. A program takes and returns all parts, laid end to end along the dimension named above; an argument that names none is the same for every part. Nothing has to cross between parts.
Inputs may be any that keep to these rules, and one draw needn't show every extreme that they name: `expert_ids`: each token names 2 different experts; among the 128 tokens of one device (aligned blocks of rows) no expert is named more than 32 times, and in every draw some expert is named exactly 32 times by some device's tokens.
All inputs are finite; a program needn't handle non-finite values.
Results may differ from the reference program's by a relative error of at most 0.0071.
Values may be sent and summed in bfloat16 or wider, within the bound.
A program may use at most 64 MiB of HBM per device.

```python
import math
import jax
import jax.numpy as jnp
import numpy as np
from jax import lax

D = 2048
FE = 512
TOP_K = 2
TOK_DEV = 128
EXPERTS = 16
TOKENS = 2048
CAP = 32
N_EP = 4
N_TP = 4


def block_levels(stream_key, shape, cuts, least, high):
    gain, own = 1.0, jax.random.fold_in(stream_key, 6)
    for dim, blocks in cuts:
        steps = jnp.exp(jax.random.uniform(jax.random.fold_in(own, dim), (blocks,), jnp.float32, least / len(cuts), high / len(cuts)))
        gain = gain * jnp.repeat(steps, shape[dim] // blocks).reshape([-1 if axis == dim else 1 for axis in range(len(shape))])
    return gain


def shared_out(key, own, number, rows, amount, top, reach, lean):
    ranking = jax.random.permutation(key, amount)
    packed, ordinary = portions_of(amount, rows * top, reach, lean, True), portions_of(amount, rows * top, reach, lean, False)
    places = jnp.arange(amount)

    def named(lengths, offset_by):
        used = int((lengths > 0).sum())
        fixed = max(1, used // 4)
        passed = fixed + (places - fixed + offset_by * (used - fixed)) % max(1, amount - fixed)
        return jnp.zeros((amount,), jnp.int32).at[ranking[jnp.where(places < fixed, places, passed)]].set(jnp.asarray(lengths, jnp.int32))

    lengths = jnp.where(number % 4 == 0, named(packed, number // 4), named(ordinary, number - number // 4 - 1))
    mixed = jax.random.permutation(jax.random.fold_in(own, 3), amount)
    donor, taker = mixed[0:amount // 2 * 2:2], mixed[1:amount // 2 * 2:2]
    room = jnp.minimum(lengths[donor] - 1, reach - lengths[taker]) // 2
    room = jnp.where((donor == ranking[0]) | (taker == ranking[0]) | (lengths[taker] == 0), 0, jnp.maximum(room, 0))
    passed = jax.random.randint(jax.random.fold_in(own, 4), (amount // 2,), 0, 1 << 20) % (room + 1)
    lengths = lengths.at[donor].add(-passed).at[taker].add(passed)
    labels = jnp.searchsorted(jnp.cumsum(lengths), jnp.arange(rows * top), side="right").astype(jnp.int32)
    listing = labels.reshape(top, rows).T
    listing = listing[jax.random.permutation(jax.random.fold_in(own, 1), rows)]
    offset_by = jax.random.randint(jax.random.fold_in(own, 2), (rows, 1), 0, top)
    return jnp.take_along_axis(listing, (jnp.arange(top)[None, :] + offset_by) % top, axis=1)


def portions_of(amount, total, most, lean, full):
    weights = [(1 << 20) // math.isqrt(rank ** lean) + 1 for rank in range(1, amount + 1)]
    largest = most if full else min(most, max(-(-total // amount), total * weights[0] // sum(weights)))
    least = 1 if total - largest >= amount - 1 else 0
    given, surplus = [largest] + [least] * (amount - 1), total - largest - least * (amount - 1)
    while surplus > 0:
        free = [i for i in range(1, amount) if given[i] < largest] or [i for i in range(1, amount) if given[i] < most]
        mass, remaining = sum([weights[i] for i in free]), surplus
        for i in free:
            addition = min(most - given[i], max(1, remaining * weights[i] // mass), surplus)
            given[i] = given[i] + addition
            surplus = surplus - addition
    return np.array(given)


def gaussian(stream_key, extent, deviation, most, split=(), held_as=jnp.bfloat16):
    result = jax.random.normal(stream_key, extent, jnp.float32) * deviation
    if len(split) > 0:
        result = block_levels(stream_key, extent, split, -0.22, 0.18) * result
    return jnp.clip(result, min=-most, max=most).astype(held_as)


def setup_inputs(seed: int = 0, part: int = 0) -> dict:
    splits = jax.random.split(jax.random.key(seed), 8)
    own_keys = jax.random.split(jax.random.fold_in(splits[7], part), 8)
    hidden_in = gaussian(own_keys[0], (TOKENS, D), 1.0, 6.0, ((0, 16),))
    expert_ids_keys = jax.random.split(jax.random.fold_in(own_keys[1], 1), TOKENS // TOK_DEV)
    expert_ids_turns = jax.random.permutation(jax.random.fold_in(own_keys[1], 3), TOKENS // TOK_DEV)
    expert_ids = jax.vmap(lambda own, number: shared_out(jax.random.fold_in(own_keys[1], 2), own, number, TOK_DEV, EXPERTS, TOP_K, CAP, 2))(expert_ids_keys, expert_ids_turns).reshape((TOKENS, TOP_K))
    route_weights = jnp.clip(jnp.exp(math.log(1.0) - 2.3025851 * jax.random.uniform(own_keys[2], (TOKENS, TOP_K), jnp.float32) ** block_levels(own_keys[2], (TOKENS, TOP_K), ((0, 16),), -0.2, 0.2)), 0.1, 1.0)
    norm_gain = jnp.clip(1.0 + 0.18 * jax.random.normal(splits[3], (D,), jnp.float32), 0.1, 1.9)
    gate_proj = gaussian(splits[4], (EXPERTS, D, FE), D ** -0.5, 0.125, ((0, 16),))
    up_proj = gaussian(splits[5], (EXPERTS, D, FE), D ** -0.5, 0.125, ((0, 16),))
    down_proj = gaussian(splits[6], (EXPERTS, FE, D), FE ** -0.5, 0.25, ((0, 16),))
    return dict(hidden_in=hidden_in, expert_ids=expert_ids, route_weights=route_weights, norm_gain=norm_gain, gate_proj=gate_proj, up_proj=up_proj, down_proj=down_proj)


def reference(hidden_in, expert_ids, route_weights, norm_gain, gate_proj, up_proj, down_proj):
    device_count = N_EP * N_TP
    as_float = hidden_in.astype(jnp.float32)
    scaled = as_float * lax.rsqrt(lax.optimization_barrier(jnp.mean(as_float * as_float, axis=-1, keepdims=True)) + 1e-06)
    normed = (scaled * norm_gain).astype(jnp.bfloat16)
    flat_ids = expert_ids.reshape(device_count, TOK_DEV * TOP_K).astype(jnp.int32)
    onehot = (flat_ids[:, :, None] == jnp.arange(EXPERTS, dtype=jnp.int32)[None, None, :]).astype(jnp.int32)
    slot_index = lax.optimization_barrier(jnp.sum((jnp.cumsum(onehot, axis=1) - onehot) * onehot, axis=2)).astype(jnp.int32)
    source = jnp.arange(device_count, dtype=jnp.int32)[:, None]
    target = (flat_ids * (device_count * CAP) + source * CAP + slot_index).reshape(-1).astype(jnp.int32)
    routed = jnp.repeat(normed, TOP_K, axis=0)
    expert_rows = jnp.zeros((EXPERTS * device_count * CAP, D), jnp.bfloat16).at[target].set(routed)
    expert_rows = expert_rows.reshape(EXPERTS, device_count * CAP, D)

    def run_expert(pieces):
        block_in, weight_gate, weight_up, weight_down = pieces
        block_float = block_in.astype(jnp.float32)
        gate_act = jnp.dot(block_float, weight_gate.astype(jnp.float32))
        up_act = jnp.dot(block_float, weight_up.astype(jnp.float32))
        hidden = (jax.nn.silu(gate_act) * up_act).astype(jnp.bfloat16)
        return jnp.dot(hidden.astype(jnp.float32), weight_down.astype(jnp.float32)).astype(jnp.bfloat16)
    expert_out = lax.map(run_expert, (expert_rows, gate_proj, up_proj, down_proj))
    picked = expert_out.reshape(-1, D)[target].astype(jnp.float32).reshape(TOKENS, TOP_K, D)
    return lax.optimization_barrier(jnp.sum(picked * route_weights[:, :, None], axis=1)).astype(jnp.bfloat16)
```

```python
import functools

import jax
import jax.numpy as jnp
from jax import lax
from jax.experimental import pallas as pl
from jax.experimental.pallas import tpu as pltpu
from jax.sharding import PartitionSpec as P

CHUNKS = 4


def slot_capacity(choose_count, token_count, expert_count):
    return max(2, 2 * choose_count * token_count // expert_count)


def pick(z, table):
    value = jnp.int32(table[0])
    for index in range(1, len(table)):
        value = jnp.where(z == index, jnp.int32(table[index]), value)
    return value


def kernel(
    n, m, cap, chunks,
    hid, ids, wts, gain, gate_hbm, up_hbm, down_hbm, out,
    ag, meta, disp, xin, res, back, part, rin_l, rin_r, acc, gate, up, down,
    w_sem, ag_s, ag_r, me_s, me_r, xd_s, xd_r, xb_s, xb_r, rs_s, rs_l, rs_r,
):
    z = lax.axis_index("ep")
    t = lax.axis_index("tp")
    tokens, width = hid.shape
    rows = m * cap
    cw = width // chunks
    choose = ids.shape[0]
    experts = n * m
    middle = jnp.logical_and(z > 0, z < n - 1)
    end = jnp.logical_or(z == 0, z == n - 1)
    by_z = [sorted(range(n), key=lambda b: (abs(b - q), b)) for q in range(n)]
    order = [pick(z, [by_z[q][s] for q in range(n)]) for s in range(n)]

    def to_ep(q):
        return {"ep": q}

    def to_tp(q):
        return {"tp": q}

    def cols(c):
        return pl.ds(c * cw, cw)

    loads = [
        pltpu.make_async_copy(gate_hbm.at[0], gate, w_sem.at[0]),
        pltpu.make_async_copy(up_hbm.at[0], up, w_sem.at[1]),
        pltpu.make_async_copy(down_hbm.at[0], down, w_sem.at[2]),
    ]
    for load in loads:
        load.start()

    barrier = pltpu.get_barrier_semaphore()

    def greet(q):
        pl.semaphore_signal(
            barrier, inc=1, device_id=q, device_id_type=pl.DeviceIdType.MESH
        )

    for d in range(1, m):
        greet(to_tp(lax.rem(t + d, m)))

    @pl.when(z > 0)
    def _():
        greet(to_ep(z - 1))

    @pl.when(z < n - 1)
    def _():
        greet(to_ep(z + 1))

    def remote(src, dst, s_sem, r_sem, dev):
        return pltpu.make_async_remote_copy(
            src_ref=src, dst_ref=dst, send_sem=s_sem, recv_sem=r_sem,
            device_id=dev, device_id_type=pl.DeviceIdType.MESH,
        )

    right, left = jnp.minimum(z + 1, n - 1), jnp.maximum(z - 1, 0)

    def ag_copy(b, c, side):
        return remote(
            ag.at[b, :, cols(c)], ag.at[b, :, cols(c)], ag_s.at[side, b, c], ag_r.at[b, c],
            to_ep(left if side == 0 else right),
        )

    def me_copy(b, side):
        return remote(
            meta.at[b], meta.at[b], me_s.at[side, b], me_r.at[b],
            to_ep(left if side == 0 else right),
        )

    def xd_copy(b, j, c):
        return remote(
            disp.at[b, j, :, cols(c)], xin.at[b, t, :, cols(c)], xd_s.at[b, j, c],
            xd_r.at[b, t, c], to_tp(j),
        )

    def xd_from(b, j, c):
        return remote(
            disp.at[b, j, :, cols(c)], xin.at[b, j, :, cols(c)], xd_s.at[b, j, c],
            xd_r.at[b, j, c], to_tp(j),
        )

    def xb_copy(b, j, c):
        return remote(
            res.at[b, j, :, cols(c)], back.at[b, t, :, cols(c)], xb_s.at[b, j, c],
            xb_r.at[b, t, c], to_tp(j),
        )

    def xb_from(b, j, c):
        return remote(
            res.at[b, j, :, cols(c)], back.at[b, j, :, cols(c)], xb_s.at[b, j, c],
            xb_r.at[b, j, c], to_tp(j),
        )

    def rs_copy(b, c, side):
        return remote(
            part.at[b, :, cols(c)], (rin_r if side == 0 else rin_l).at[b, :, cols(c)],
            rs_s.at[b, c], (rs_r if side == 0 else rs_l).at[b, c],
            to_ep(left if side == 0 else right),
        )

    def rs_send(b, c):
        @pl.when(b > z)
        def _():
            rs_copy(b, c, 1).start()

        @pl.when(b < z)
        def _():
            rs_copy(b, c, 0).start()

    expert_row = lax.broadcasted_iota(jnp.int32, (experts, tokens), 0)
    named = [(expert_row == ids[k : k + 1, :]).astype(jnp.float32) for k in range(choose)]
    total = named[0]
    for k in range(1, choose):
        total = total + named[k]
    before = (
        lax.broadcasted_iota(jnp.int32, (tokens, tokens), 0)
        < lax.broadcasted_iota(jnp.int32, (tokens, tokens), 1)
    ).astype(jnp.bfloat16)
    counts = jnp.dot(total.astype(jnp.bfloat16), before, preferred_element_type=jnp.float32)
    first = expert_row.astype(jnp.float32) * cap + counts
    lines = [jnp.sum(named[k] * first, axis=0, keepdims=True) for k in range(choose)]
    lines += [wts[k : k + 1, :] for k in range(choose)]
    lines.append(jnp.zeros((meta.shape[1] - 2 * choose, tokens), jnp.float32))
    meta[z] = jnp.concatenate(lines, axis=0)

    hidden = hid[...].astype(jnp.float32)
    scale = lax.rsqrt(jnp.mean(hidden * hidden, axis=-1, keepdims=True) + 1e-06)
    ag[z] = (hidden * scale * gain[...]).astype(jnp.bfloat16)

    partners = (m - 1) + (z > 0).astype(jnp.int32) + (z < n - 1).astype(jnp.int32)
    pl.semaphore_wait(barrier, partners)

    @pl.when(z > 0)
    def _():
        me_copy(z, 0).start()

    @pl.when(z < n - 1)
    def _():
        me_copy(z, 1).start()

    for c in range(chunks):
        @pl.when(z > 0)
        def _(c=c):
            ag_copy(z, c, 0).start()

        @pl.when(z < n - 1)
        def _(c=c):
            ag_copy(z, c, 1).start()

    def receive(b, c):
        if c == 0:
            me_copy(b, 0).wait_recv()
        ag_copy(b, c, 0).wait_recv()

    def forward(s):
        b = order[s]

        @pl.when(middle)
        def _():
            for c in range(chunks):
                receive(b, c)

                @pl.when(b < z)
                def _(c=c):
                    if c == 0:
                        me_copy(b, 1).start()
                    ag_copy(b, c, 1).start()

                @pl.when(b > z)
                def _(c=c):
                    if c == 0:
                        me_copy(b, 0).start()
                    ag_copy(b, c, 0).start()

    def slot_row():
        row = lax.broadcasted_iota(jnp.int32, (rows, tokens), 0) + z * rows
        return row.astype(jnp.float32)

    def dispatch(s, wait):
        b = order[s]
        select = None
        for c in range(chunks):
            if wait:
                receive(b, c)
            if select is None:
                info = meta[b]
                row = slot_row()
                select = jnp.zeros((rows, tokens), jnp.float32)
                for k in range(choose):
                    select = select + (row == info[k : k + 1, :]).astype(jnp.float32)
                select = select.astype(jnp.bfloat16)
            sent = jnp.dot(select, ag[b, :, cols(c)], preferred_element_type=jnp.float32)
            disp[b, :, :, cols(c)] = sent.astype(jnp.bfloat16).reshape(m, cap, cw)
            for d in range(m - 1, 0, -1):
                xd_copy(b, lax.rem(t + d, m), c).start()
            xin[b, t, :, cols(c)] = disp[b, t, :, cols(c)]

    def experts_step(s):
        b = order[s]
        if s == 0:
            loads[0].wait()
            loads[1].wait()
        gate_act = jnp.zeros((rows, gate.shape[1]), jnp.float32)
        up_act = jnp.zeros((rows, gate.shape[1]), jnp.float32)
        for c in range(chunks):
            for d in range(1, m):
                xd_from(b, lax.rem(t + d, m), c).wait_recv()
            block = xin[b, :, :, cols(c)].reshape(rows, cw)
            gate_act += jnp.dot(block, gate[cols(c), :], preferred_element_type=jnp.float32)
            up_act += jnp.dot(block, up[cols(c), :], preferred_element_type=jnp.float32)
        act = (gate_act / (1.0 + jnp.exp(-gate_act)) * up_act).astype(jnp.bfloat16)
        if s == 0:
            loads[2].wait()
        for c in range(chunks):
            made = jnp.dot(act, down[:, cols(c)], preferred_element_type=jnp.float32)
            res[b, :, :, cols(c)] = made.astype(jnp.bfloat16).reshape(m, cap, cw)
            for d in range(m - 1, 0, -1):
                xb_copy(b, lax.rem(t + d, m), c).start()
            back[b, t, :, cols(c)] = res[b, t, :, cols(c)]

    def combine(s):
        b = order[s]
        info = meta[b]
        row = slot_row()
        mix = jnp.zeros((rows, tokens), jnp.float32)
        for k in range(choose):
            mix = mix + jnp.where(
                row == info[k : k + 1, :], info[choose + k : choose + k + 1, :], 0.0
            )
        mix = jnp.transpose(mix).astype(jnp.bfloat16)
        for c in range(chunks):
            for d in range(1, m):
                xb_from(b, lax.rem(t + d, m), c).wait_recv()
            block = back[b, :, :, cols(c)].reshape(rows, cw)
            value = jnp.dot(mix, block, preferred_element_type=jnp.float32)
            if s == 0:
                acc[:, cols(c)] = value
            else:
                part[b, :, cols(c)] = value.astype(jnp.bfloat16)

                @pl.when(end)
                def _(c=c):
                    rs_send(b, c)

    dispatch(0, False)
    experts_step(0)
    for s in (1, 2):
        if s < n:
            forward(s)

    def ready(s, where):
        if s < n:
            @pl.when(where)
            def _():
                dispatch(s, where is end)

    ready(1, middle)
    ready(2, middle)
    ready(1, end)
    combine(0)
    for s in range(1, n):
        experts_step(s)
        combine(s)
        if s + 2 < n:
            forward(s + 2)
        ready(s + 2, middle)
        ready(s + 1, end)

    def due(q):
        return sorted(
            [b for b in range(n) if b != q],
            key=lambda b: (b, q) if b > q else (n - 1 - b, n - 1 - q),
        )

    dues = [due(q) for q in range(n)]
    later = [pick(z, [dues[q][s] for q in range(n)]) for s in range(n - 1)]

    @pl.when(middle)
    def _():
        def add(b, c):
            @pl.when(b > z)
            def _():
                rs_copy(b, c, 1).wait_recv()
                part[b, :, cols(c)] = part[b, :, cols(c)] + rin_l[b, :, cols(c)]

            @pl.when(b < z)
            def _():
                rs_copy(b, c, 0).wait_recv()
                part[b, :, cols(c)] = part[b, :, cols(c)] + rin_r[b, :, cols(c)]

            rs_send(b, c)

        for b in later[:-2]:
            for c in range(chunks):
                add(b, c)
        for c in range(chunks):
            for b in later[-2:]:
                add(b, c)

    for c in range(chunks):
        @pl.when(z > 0)
        def _(c=c):
            rs_copy(z, c, 1).wait_recv()
            acc[:, cols(c)] = acc[:, cols(c)] + rin_l[z, :, cols(c)].astype(jnp.float32)

        @pl.when(z < n - 1)
        def _(c=c):
            rs_copy(z, c, 0).wait_recv()
            acc[:, cols(c)] = acc[:, cols(c)] + rin_r[z, :, cols(c)].astype(jnp.float32)

        out[:, cols(c)] = acc[:, cols(c)].astype(jnp.bfloat16)

    for s in range(n):
        b = order[s]

        @pl.when(jnp.logical_and(b >= z, z > 0))
        def _(b=b):
            me_copy(b, 0).wait_send()
            for c in range(chunks):
                ag_copy(b, c, 0).wait_send()

        @pl.when(jnp.logical_and(b <= z, z < n - 1))
        def _(b=b):
            me_copy(b, 1).wait_send()
            for c in range(chunks):
                ag_copy(b, c, 1).wait_send()

        for c in range(chunks):
            for d in range(1, m):
                xd_copy(b, lax.rem(t + d, m), c).wait_send()
                xb_copy(b, lax.rem(t + d, m), c).wait_send()
            if s > 0:
                rs_copy(b, c, 0).wait_send()


def fused(n, m, cap, hidden_in, expert_ids, route_weights, norm_gain, gate_proj, up_proj, down_proj):
    tokens, width = hidden_in.shape
    units = gate_proj.shape[2]
    chunks = CHUNKS
    choose = expert_ids.shape[1]
    lines = -(-2 * choose // 8) * 8
    bf = jnp.bfloat16
    dma = pltpu.SemaphoreType.DMA
    vmem = pl.BlockSpec(memory_space=pltpu.VMEM)
    hbm = pl.BlockSpec(memory_space=pl.ANY)
    return pl.pallas_call(
        functools.partial(kernel, n, m, cap, chunks),
        out_shape=jax.ShapeDtypeStruct((tokens, width), bf),
        in_specs=[vmem] * 4 + [hbm] * 3,
        out_specs=vmem,
        scratch_shapes=[
            pltpu.VMEM((n, tokens, width), bf),
            pltpu.VMEM((n, lines, tokens), jnp.float32),
            pltpu.VMEM((n, m, cap, width), bf),
            pltpu.VMEM((n, m, cap, width), bf),
            pltpu.VMEM((n, m, cap, width), bf),
            pltpu.VMEM((n, m, cap, width), bf),
            pltpu.VMEM((n, tokens, width), bf),
            pltpu.VMEM((n, tokens, width), bf),
            pltpu.VMEM((n, tokens, width), bf),
            pltpu.VMEM((tokens, width), jnp.float32),
            pltpu.VMEM((width, units), bf),
            pltpu.VMEM((width, units), bf),
            pltpu.VMEM((units, width), bf),
            dma((3,)),
            dma((2, n, chunks)), dma((n, chunks)),
            dma((2, n)), dma((n,)),
            dma((n, m, chunks)), dma((n, m, chunks)),
            dma((n, m, chunks)), dma((n, m, chunks)),
            dma((n, chunks)), dma((n, chunks)), dma((n, chunks)),
        ],
        compiler_params=pltpu.CompilerParams(
            collective_id=0, has_side_effects=True, vmem_limit_bytes=48 * 1024 * 1024
        ),
        name="experts",
    )(
        hidden_in, expert_ids.T, route_weights.T, norm_gain.reshape(1, -1),
        gate_proj, up_proj, down_proj,
    )


def by_slots(capacity, hidden_in, expert_ids, route_weights, norm_gain, gate_proj, up_proj, down_proj):
    token_count = hidden_in.shape[0]
    model_width = hidden_in.shape[1]
    choose_count = expert_ids.shape[1]
    expert_count = lax.axis_size("ep") * lax.axis_size("tp")
    as_float = hidden_in.astype(jnp.float32)
    scaled = as_float * lax.rsqrt(jnp.mean(as_float * as_float, axis=-1, keepdims=True) + 1e-06)
    normed = (scaled * norm_gain).astype(jnp.bfloat16)
    flat_ids = expert_ids.reshape(-1)
    onehot = (flat_ids[:, None] == jnp.arange(expert_count, dtype=jnp.int32)[None, :]).astype(
        jnp.int32
    )
    slot_index = jnp.sum((jnp.cumsum(onehot, axis=0) - onehot) * onehot, axis=1)
    target = flat_ids * capacity + slot_index
    routed = jnp.repeat(normed, choose_count, axis=0)
    buffer = jnp.zeros((expert_count * capacity, model_width), jnp.bfloat16).at[target].set(routed)
    buffer = buffer.reshape(expert_count, capacity, model_width)
    arrived = lax.all_to_all(buffer, ("ep", "tp"), split_axis=0, concat_axis=0, tiled=True)
    shape_in = arrived.shape
    block_in = arrived.reshape(-1, model_width)
    gate_act = jnp.dot(block_in, gate_proj[0], preferred_element_type=jnp.float32)
    up_act = jnp.dot(block_in, up_proj[0], preferred_element_type=jnp.float32)
    hidden = (jax.nn.silu(gate_act) * up_act).astype(jnp.bfloat16)
    result = jnp.dot(hidden, down_proj[0], preferred_element_type=jnp.float32).astype(jnp.bfloat16)
    results = result.reshape(shape_in)
    returned = lax.all_to_all(results, ("ep", "tp"), split_axis=0, concat_axis=0, tiled=True)
    picked = returned.reshape(-1, model_width)[target].astype(jnp.float32)
    picked = picked.reshape(token_count, choose_count, model_width)
    return jnp.sum(picked * route_weights[:, :, None], axis=1).astype(jnp.bfloat16)


def body(hidden_in, expert_ids, *rest):
    n, m = lax.axis_size("ep"), lax.axis_size("tp")
    tokens = hidden_in.shape[0]
    cap = slot_capacity(expert_ids.shape[1], tokens, n * m)
    if n > 2 and m * cap >= tokens and cap % 16 == 0:
        return fused(n, m, cap, hidden_in, expert_ids, *rest)
    return by_slots(cap, hidden_in, expert_ids, *rest)


def solution(mesh):
    return jax.shard_map(
        body,
        mesh=mesh,
        in_specs=(
            P(("grp", "ep", "tp"), None),
            P(("grp", "ep", "tp"), None),
            P(("grp", "ep", "tp"), None),
            P(),
            P(("ep", "tp"), None, None),
            P(("ep", "tp"), None, None),
            P(("ep", "tp"), None, None),
        ),
        out_specs=P(("grp", "ep", "tp"), None),
        check_vma=False,
    )
```

```python
import functools

import jax
import jax.numpy as jnp
from jax import lax
from jax.experimental import pallas as pl
from jax.experimental.pallas import tpu as pltpu
from jax.sharding import PartitionSpec as P

Z_CHUNKS = 2
X_CHUNKS = 1


def slot_capacity(choose_count, token_count, expert_count):
    return max(2, 2 * choose_count * token_count // expert_count)


def pick(z, table):
    value = jnp.int32(table[0])
    for index in range(1, len(table)):
        value = jnp.where(z == index, jnp.int32(table[index]), value)
    return value


def kernel(
    n, m, cap, chunks, xchunks,
    hid, ids, wts, gain, gate_hbm, up_hbm, down_hbm, out,
    ag, meta, disp, xin, res, back, part, rin_l, rin_r, acc, gate, up, down,
    w_sem, ag_s, ag_r, me_s, me_r, xd_s, xd_r, xb_s, xb_r, rs_s, rs_l, rs_r,
):
    z = lax.axis_index("ep")
    t = lax.axis_index("tp")
    tokens, width = hid.shape
    rows = m * cap
    cw = width // chunks
    xw = width // xchunks
    ratio = chunks // xchunks
    choose = ids.shape[0]
    experts = n * m
    middle = jnp.logical_and(z > 0, z < n - 1)
    end = jnp.logical_or(z == 0, z == n - 1)
    by_z = [sorted(range(n), key=lambda b: (abs(b - q), b)) for q in range(n)]
    order = [pick(z, [by_z[q][s] for q in range(n)]) for s in range(n)]

    def to_ep(q):
        return {"ep": q}

    def to_tp(q):
        return {"tp": q}

    def cols(c):
        return pl.ds(c * cw, cw)

    def xcols(q):
        return pl.ds(q * xw, xw)

    loads = [
        pltpu.make_async_copy(gate_hbm.at[0], gate, w_sem.at[0]),
        pltpu.make_async_copy(up_hbm.at[0], up, w_sem.at[1]),
        pltpu.make_async_copy(down_hbm.at[0], down, w_sem.at[2]),
    ]
    for load in loads:
        load.start()

    barrier = pltpu.get_barrier_semaphore()

    def greet(q):
        pl.semaphore_signal(
            barrier, inc=1, device_id=q, device_id_type=pl.DeviceIdType.MESH
        )

    for d in range(1, m):
        greet(to_tp(lax.rem(t + d, m)))

    @pl.when(z > 0)
    def _():
        greet(to_ep(z - 1))

    @pl.when(z < n - 1)
    def _():
        greet(to_ep(z + 1))

    def remote(src, dst, s_sem, r_sem, dev):
        return pltpu.make_async_remote_copy(
            src_ref=src, dst_ref=dst, send_sem=s_sem, recv_sem=r_sem,
            device_id=dev, device_id_type=pl.DeviceIdType.MESH,
        )

    right, left = jnp.minimum(z + 1, n - 1), jnp.maximum(z - 1, 0)

    def ag_copy(b, c, side):
        return remote(
            ag.at[b, c], ag.at[b, c], ag_s.at[side, b, c], ag_r.at[b, c],
            to_ep(left if side == 0 else right),
        )

    def me_copy(b, side):
        return remote(
            meta.at[b], meta.at[b], me_s.at[side, b], me_r.at[b],
            to_ep(left if side == 0 else right),
        )

    def xd_copy(b, j, c):
        return remote(
            disp.at[b, c, j], xin.at[b, c, t], xd_s.at[b, j, c],
            xd_r.at[b, t, c], to_tp(j),
        )

    def xd_from(b, j, c):
        return remote(
            disp.at[b, c, j], xin.at[b, c, j], xd_s.at[b, j, c],
            xd_r.at[b, j, c], to_tp(j),
        )

    def xb_copy(b, j, c):
        return remote(
            res.at[b, c, j], back.at[b, c, t], xb_s.at[b, j, c],
            xb_r.at[b, t, c], to_tp(j),
        )

    def xb_from(b, j, c):
        return remote(
            res.at[b, c, j], back.at[b, c, j], xb_s.at[b, j, c],
            xb_r.at[b, j, c], to_tp(j),
        )

    def rs_copy(b, c, side):
        return remote(
            part.at[b, c], (rin_r if side == 0 else rin_l).at[b, c],
            rs_s.at[b, c], (rs_r if side == 0 else rs_l).at[b, c],
            to_ep(left if side == 0 else right),
        )

    def rs_send(b, c):
        @pl.when(b > z)
        def _():
            rs_copy(b, c, 1).start()

        @pl.when(b < z)
        def _():
            rs_copy(b, c, 0).start()

    expert_row = lax.broadcasted_iota(jnp.int32, (experts, tokens), 0)
    named = [(expert_row == ids[k : k + 1, :]).astype(jnp.float32) for k in range(choose)]
    total = named[0]
    for k in range(1, choose):
        total = total + named[k]
    before = (
        lax.broadcasted_iota(jnp.int32, (tokens, tokens), 0)
        < lax.broadcasted_iota(jnp.int32, (tokens, tokens), 1)
    ).astype(jnp.bfloat16)
    counts = jnp.dot(total.astype(jnp.bfloat16), before, preferred_element_type=jnp.float32)
    first = expert_row.astype(jnp.float32) * cap + counts
    lines = [jnp.sum(named[k] * first, axis=0, keepdims=True) for k in range(choose)]
    lines += [wts[k : k + 1, :] for k in range(choose)]
    lines.append(jnp.zeros((meta.shape[1] - 2 * choose, tokens), jnp.float32))
    meta[z] = jnp.concatenate(lines, axis=0)

    hidden = hid[...].astype(jnp.float32)
    scale = lax.rsqrt(jnp.mean(hidden * hidden, axis=-1, keepdims=True) + 1e-06)
    for c in range(chunks):
        normed = hidden[:, c * cw : (c + 1) * cw] * scale * gain[:, cols(c)]
        ag[z, c] = normed.astype(jnp.bfloat16)

    partners = (m - 1) + (z > 0).astype(jnp.int32) + (z < n - 1).astype(jnp.int32)
    pl.semaphore_wait(barrier, partners)

    @pl.when(z > 0)
    def _():
        me_copy(z, 0).start()

    @pl.when(z < n - 1)
    def _():
        me_copy(z, 1).start()

    for c in range(chunks):
        @pl.when(z > 0)
        def _(c=c):
            ag_copy(z, c, 0).start()

        @pl.when(z < n - 1)
        def _(c=c):
            ag_copy(z, c, 1).start()

    def receive(b, c):
        if c == 0:
            me_copy(b, 0).wait_recv()
        ag_copy(b, c, 0).wait_recv()

    def forward(s):
        b = order[s]
        for c in range(chunks):
            receive(b, c)

            @pl.when(b < z)
            def _(c=c):
                if c == 0:
                    me_copy(b, 1).start()
                ag_copy(b, c, 1).start()

            @pl.when(b > z)
            def _(c=c):
                if c == 0:
                    me_copy(b, 0).start()
                ag_copy(b, c, 0).start()

    def slot_row():
        row = lax.broadcasted_iota(jnp.int32, (rows, tokens), 0) + z * rows
        return row.astype(jnp.float32)

    def dispatch(s, wait):
        b = order[s]
        select = None
        for c in range(chunks):
            if wait:
                receive(b, c)
            if select is None:
                info = meta[b]
                row = slot_row()
                select = jnp.zeros((rows, tokens), jnp.float32)
                for k in range(choose):
                    select = select + (row == info[k : k + 1, :]).astype(jnp.float32)
                select = select.astype(jnp.bfloat16)
            sent = jnp.dot(select, ag[b, c], preferred_element_type=jnp.float32)
            q = c // ratio
            inner = pl.ds((c % ratio) * cw, cw)
            disp[b, q, :, :, inner] = sent.astype(jnp.bfloat16).reshape(m, cap, cw)
            if (c + 1) % ratio == 0:
                for d in range(m - 1, 0, -1):
                    xd_copy(b, lax.rem(t + d, m), q).start()
                xin[b, q, t] = disp[b, q, t]

    def experts_step(s):
        b = order[s]
        if s == 0:
            loads[0].wait()
            loads[1].wait()
        gate_act = jnp.zeros((rows, gate.shape[1]), jnp.float32)
        up_act = jnp.zeros((rows, gate.shape[1]), jnp.float32)
        for q in range(xchunks):
            for d in range(1, m):
                xd_from(b, lax.rem(t + d, m), q).wait_recv()
            block = xin[b, q].reshape(rows, xw)
            gate_act += jnp.dot(block, gate[xcols(q), :], preferred_element_type=jnp.float32)
            up_act += jnp.dot(block, up[xcols(q), :], preferred_element_type=jnp.float32)
        act = (gate_act / (1.0 + jnp.exp(-gate_act)) * up_act).astype(jnp.bfloat16)
        if s == 0:
            loads[2].wait()
        for q in range(xchunks):
            made = jnp.dot(act, down[:, xcols(q)], preferred_element_type=jnp.float32)
            res[b, q] = made.astype(jnp.bfloat16).reshape(m, cap, xw)
            for d in range(m - 1, 0, -1):
                xb_copy(b, lax.rem(t + d, m), q).start()
            back[b, q, t] = res[b, q, t]

    def combine(s):
        b = order[s]
        info = meta[b]
        row = slot_row()
        mix = jnp.zeros((rows, tokens), jnp.float32)
        for k in range(choose):
            mix = mix + jnp.where(
                row == info[k : k + 1, :], info[choose + k : choose + k + 1, :], 0.0
            )
        mix = jnp.transpose(mix).astype(jnp.bfloat16)
        for c in range(chunks):
            q = c // ratio
            if c % ratio == 0:
                for d in range(1, m):
                    xb_from(b, lax.rem(t + d, m), q).wait_recv()
            block = back[b, q, :, :, pl.ds((c % ratio) * cw, cw)].reshape(rows, cw)
            value = jnp.dot(mix, block, preferred_element_type=jnp.float32)
            if s == 0:
                acc[:, cols(c)] = value
            else:
                part[b, c] = value.astype(jnp.bfloat16)

                @pl.when(end)
                def _(c=c, b=b):
                    rs_send(b, c)

    dispatch(0, False)
    experts_step(0)

    @pl.when(end)
    def _():
        for s in range(1, n):
            dispatch(s, True)
            if s == 1:
                combine(0)
            experts_step(s)
            combine(s)

    @pl.when(middle)
    def _():
        forward(1)
        forward(2)
        dispatch(1, False)
        dispatch(2, False)
        combine(0)
        for s in range(1, n):
            experts_step(s)
            if s + 2 < n:
                forward(s + 2)
                dispatch(s + 2, False)
            if s > 1:
                combine(s - 1)
        combine(n - 1)

    def due(q):
        return sorted(
            [b for b in range(n) if b != q],
            key=lambda b: (b, q) if b > q else (n - 1 - b, n - 1 - q),
        )

    dues = [due(q) for q in range(n)]
    later = [pick(z, [dues[q][s] for q in range(n)]) for s in range(n - 1)]

    @pl.when(middle)
    def _():
        def add(b, c):
            @pl.when(b > z)
            def _():
                rs_copy(b, c, 1).wait_recv()
                part[b, c] = part[b, c] + rin_l[b, c]

            @pl.when(b < z)
            def _():
                rs_copy(b, c, 0).wait_recv()
                part[b, c] = part[b, c] + rin_r[b, c]

            rs_send(b, c)

        for b in later[:-2]:
            for c in range(chunks):
                add(b, c)
        for c in range(chunks):
            for b in later[-2:]:
                add(b, c)

    for c in range(chunks):
        @pl.when(z > 0)
        def _(c=c):
            rs_copy(z, c, 1).wait_recv()
            acc[:, cols(c)] = acc[:, cols(c)] + rin_l[z, c].astype(jnp.float32)

        @pl.when(z < n - 1)
        def _(c=c):
            rs_copy(z, c, 0).wait_recv()
            acc[:, cols(c)] = acc[:, cols(c)] + rin_r[z, c].astype(jnp.float32)

        out[:, cols(c)] = acc[:, cols(c)].astype(jnp.bfloat16)

    for s in range(n):
        b = order[s]

        @pl.when(jnp.logical_and(b >= z, z > 0))
        def _(b=b):
            me_copy(b, 0).wait_send()
            for c in range(chunks):
                ag_copy(b, c, 0).wait_send()

        @pl.when(jnp.logical_and(b <= z, z < n - 1))
        def _(b=b):
            me_copy(b, 1).wait_send()
            for c in range(chunks):
                ag_copy(b, c, 1).wait_send()

        for c in range(chunks):
            if s > 0:
                rs_copy(b, c, 0).wait_send()
        for q in range(xchunks):
            for d in range(1, m):
                xd_copy(b, lax.rem(t + d, m), q).wait_send()
                xb_copy(b, lax.rem(t + d, m), q).wait_send()


def fused(n, m, cap, hidden_in, expert_ids, route_weights, norm_gain, gate_proj, up_proj, down_proj):
    tokens, width = hidden_in.shape
    units = gate_proj.shape[2]
    chunks, xchunks = Z_CHUNKS, X_CHUNKS
    cw, xw = width // chunks, width // xchunks
    choose = expert_ids.shape[1]
    lines = -(-2 * choose // 8) * 8
    bf = jnp.bfloat16
    dma = pltpu.SemaphoreType.DMA
    vmem = pl.BlockSpec(memory_space=pltpu.VMEM)
    hbm = pl.BlockSpec(memory_space=pl.ANY)
    return pl.pallas_call(
        functools.partial(kernel, n, m, cap, chunks, xchunks),
        out_shape=jax.ShapeDtypeStruct((tokens, width), bf),
        in_specs=[vmem] * 4 + [hbm] * 3,
        out_specs=vmem,
        scratch_shapes=[
            pltpu.VMEM((n, chunks, tokens, cw), bf),
            pltpu.VMEM((n, lines, tokens), jnp.float32),
            pltpu.VMEM((n, xchunks, m, cap, xw), bf),
            pltpu.VMEM((n, xchunks, m, cap, xw), bf),
            pltpu.VMEM((n, xchunks, m, cap, xw), bf),
            pltpu.VMEM((n, xchunks, m, cap, xw), bf),
            pltpu.VMEM((n, chunks, tokens, cw), bf),
            pltpu.VMEM((n, chunks, tokens, cw), bf),
            pltpu.VMEM((n, chunks, tokens, cw), bf),
            pltpu.VMEM((tokens, width), jnp.float32),
            pltpu.VMEM((width, units), bf),
            pltpu.VMEM((width, units), bf),
            pltpu.VMEM((units, width), bf),
            dma((3,)),
            dma((2, n, chunks)), dma((n, chunks)),
            dma((2, n)), dma((n,)),
            dma((n, m, xchunks)), dma((n, m, xchunks)),
            dma((n, m, xchunks)), dma((n, m, xchunks)),
            dma((n, chunks)), dma((n, chunks)), dma((n, chunks)),
        ],
        compiler_params=pltpu.CompilerParams(
            collective_id=0, has_side_effects=True, vmem_limit_bytes=48 * 1024 * 1024
        ),
        name="experts",
    )(
        hidden_in, expert_ids.T, route_weights.T, norm_gain.reshape(1, -1),
        gate_proj, up_proj, down_proj,
    )


def by_slots(capacity, hidden_in, expert_ids, route_weights, norm_gain, gate_proj, up_proj, down_proj):
    token_count = hidden_in.shape[0]
    model_width = hidden_in.shape[1]
    choose_count = expert_ids.shape[1]
    expert_count = lax.axis_size("ep") * lax.axis_size("tp")
    as_float = hidden_in.astype(jnp.float32)
    scaled = as_float * lax.rsqrt(jnp.mean(as_float * as_float, axis=-1, keepdims=True) + 1e-06)
    normed = (scaled * norm_gain).astype(jnp.bfloat16)
    flat_ids = expert_ids.reshape(-1)
    onehot = (flat_ids[:, None] == jnp.arange(expert_count, dtype=jnp.int32)[None, :]).astype(
        jnp.int32
    )
    slot_index = jnp.sum((jnp.cumsum(onehot, axis=0) - onehot) * onehot, axis=1)
    target = flat_ids * capacity + slot_index
    routed = jnp.repeat(normed, choose_count, axis=0)
    buffer = jnp.zeros((expert_count * capacity, model_width), jnp.bfloat16).at[target].set(routed)
    buffer = buffer.reshape(expert_count, capacity, model_width)
    arrived = lax.all_to_all(buffer, ("ep", "tp"), split_axis=0, concat_axis=0, tiled=True)
    shape_in = arrived.shape
    block_in = arrived.reshape(-1, model_width)
    gate_act = jnp.dot(block_in, gate_proj[0], preferred_element_type=jnp.float32)
    up_act = jnp.dot(block_in, up_proj[0], preferred_element_type=jnp.float32)
    hidden = (jax.nn.silu(gate_act) * up_act).astype(jnp.bfloat16)
    result = jnp.dot(hidden, down_proj[0], preferred_element_type=jnp.float32).astype(jnp.bfloat16)
    results = result.reshape(shape_in)
    returned = lax.all_to_all(results, ("ep", "tp"), split_axis=0, concat_axis=0, tiled=True)
    picked = returned.reshape(-1, model_width)[target].astype(jnp.float32)
    picked = picked.reshape(token_count, choose_count, model_width)
    return jnp.sum(picked * route_weights[:, :, None], axis=1).astype(jnp.bfloat16)


def body(hidden_in, expert_ids, *rest):
    n, m = lax.axis_size("ep"), lax.axis_size("tp")
    tokens = hidden_in.shape[0]
    cap = slot_capacity(expert_ids.shape[1], tokens, n * m)
    if n > 2 and m * cap >= tokens and cap % 16 == 0:
        return fused(n, m, cap, hidden_in, expert_ids, *rest)
    return by_slots(cap, hidden_in, expert_ids, *rest)


def solution(mesh):
    return jax.shard_map(
        body,
        mesh=mesh,
        in_specs=(
            P(("grp", "ep", "tp"), None),
            P(("grp", "ep", "tp"), None),
            P(("grp", "ep", "tp"), None),
            P(),
            P(("ep", "tp"), None, None),
            P(("ep", "tp"), None, None),
            P(("ep", "tp"), None, None),
        ),
        out_specs=P(("grp", "ep", "tp"), None),
        check_vma=False,
    )
```
